32 devices in a mesh: sp: 8 (over z, y), tp: 4 (over x, core).
Axes of the slice: x: 2, y: 2, z: 4, core: 2. Of those that a mesh axis runs over, the one named last changes fastest.
Arguments:
- expert_input: bfloat16 [3072, 2048], P('sp'), may hold values from -6 to 6
- cotangent: bfloat16 [3072, 2048], P('sp'), may hold values from -6 to 6
- routes: int32 [3072, 2], P('sp'), may hold values from 0 to 7, all different within a row; in each aligned block of 384 rows (0 to 383, 384 to 767, ...) at most 144 rows name the same one
- route_weight: float32 [3072, 2], P('sp'), may hold values from 0.2 to 2.5
- expert_gate: bfloat16 [8, 2048, 1024], P('sp', None, 'tp'), may hold values from -0.125 to 0.125
- expert_up: bfloat16 [8, 2048, 1024], P('sp', None, 'tp'), may hold values from -0.125 to 0.125
- expert_down: bfloat16 [8, 1024, 2048], P('sp', 'tp'), may hold values from -0.1875 to 0.1875
- conv_out: bfloat16 [3072, 1024], P('sp', 'tp'), may hold values from -14 to 14
- conv_value: bfloat16 [3072, 1024], P('sp', 'tp'), may hold values from -6 to 6
- conv_gate: bfloat16 [3072, 1024], P('sp', 'tp'), may hold values from -6 to 6
- conv_taps: float32 [31, 1024], P(None, 'tp'), may hold values from -1 to 1
- norm_gain: float32 [1024], P('tp'), may hold values from 0.1 to 1.9
- norm_bias: float32 [1024], P('tp'), may hold values from -3 to 3
- out_weight: bfloat16 [1024, 2048], P('tp'), may hold values from -0.1875 to 0.1875
Outputs:
- gate_grad: float32 [8, 2048, 1024], P('sp', None, 'tp')
- up_grad: float32 [8, 2048, 1024], P('sp', None, 'tp')
- down_grad: float32 [8, 1024, 2048], P('sp', 'tp')
- resid_grad: bfloat16 [3072, 2048], P('sp')
- out_weight_grad: float32 [1024, 2048], P('tp', 'sp')
- value_grad: bfloat16 [3072, 1024], P('sp', 'tp')
- gate_in_grad: bfloat16 [3072, 1024], P('sp', 'tp')
The draws below stay inside these ranges and needn't reach their ends.
Inputs may be any that keep to these rules, and one draw needn't show every extreme that they name: `routes`: each token names 2 different experts. In each aligned block of 384 tokens no expert is named by more than 144 tokens, and in every draw some block has an expert named by exactly 144 tokens.
All inputs are finite; a program needn't handle non-finite values.
Results may differ from the reference program's by a relative error of at most 0.018.
Values may be sent and summed in bfloat16 or wider, within the bound.
No kernel may reach another device: no remote copies, remote signals or barrier semaphores. Data moves between devices by JAX's collectives and lax.ppermute only.
A program may use at most 128 MiB of HBM per device.

```python
import math
import jax
import jax.numpy as jnp
import numpy as np
from jax import lax

D = 2048
CW = 1024
FF = 1024
KW = 31
TOP = 2
TOK_DEV = 384
TOKENS = 3072
EXPERTS = 8
CAP = 144
FGROUP = 256
N_SP = 8
N_TP = 4


def draw_conv_out(key, part):
    first_key = jax.random.fold_in(jax.random.fold_in(key, 11), 0)
    column = jnp.arange(CW, dtype=jnp.float32) / CW
    col_scale = 0.3 * jnp.exp(jnp.log(10.0) * column)[None, :]
    values = jnp.clip(jax.random.normal(first_key, (TOKENS, CW), jnp.float32), -4.0, 4.0) * col_scale
    return values.astype(jnp.bfloat16)


def spiked(array, rng, source, target, parts, factor):
    def block_of(axis_at):
        return (jnp.arange(array.shape[axis_at]) // (array.shape[axis_at] // parts)).reshape((-1,) + (1,) * (array.ndim - 1 - axis_at))

    near = jax.random.permutation(rng, parts)[block_of(target)]
    other_side = (block_of(target) + parts // 2) % parts
    return jnp.where((block_of(source) == near) | (block_of(source) == other_side), factor * array, array)


def levels(stream_key, dims, pieces, low, largest):
    loudness, own = 1.0, jax.random.fold_in(stream_key, 6)
    for position, parts in pieces:
        steps = jnp.exp(jax.random.uniform(jax.random.fold_in(own, position), (parts,), jnp.float32, low / len(pieces), largest / len(pieces)))
        loudness = loudness * jnp.repeat(steps, dims[position] // parts).reshape([-1 if axis == position else 1 for axis in range(len(dims))])
    return loudness


def assign_block(rng, own, number, rows, number_of, top, most, skew):
    order = jax.random.permutation(rng, number_of)
    crowded, usual = load_shares(number_of, rows * top, most, skew, True), load_shares(number_of, rows * top, most, skew, False)
    places = jnp.arange(number_of)

    def named(tallies, rotation):
        used = int((tallies > 0).sum())
        fixed = max(1, used // 4)
        moved = fixed + (places - fixed + rotation * (used - fixed)) % max(1, number_of - fixed)
        return jnp.zeros((number_of,), jnp.int32).at[order[jnp.where(places < fixed, places, moved)]].set(jnp.asarray(tallies, jnp.int32))

    tallies = jnp.where(number % 4 == 0, named(crowded, number // 4), named(usual, number - number // 4 - 1))
    mixed = jax.random.permutation(jax.random.fold_in(own, 3), number_of)
    donor, taker = mixed[0:number_of // 2 * 2:2], mixed[1:number_of // 2 * 2:2]
    slack = jnp.minimum(tallies[donor] - 1, most - tallies[taker]) // 2
    slack = jnp.where((donor == order[0]) | (taker == order[0]) | (tallies[taker] == 0), 0, jnp.maximum(slack, 0))
    moved = jax.random.randint(jax.random.fold_in(own, 4), (number_of // 2,), 0, 1 << 20) % (slack + 1)
    tallies = tallies.at[donor].add(-moved).at[taker].add(moved)
    items = jnp.searchsorted(jnp.cumsum(tallies), jnp.arange(rows * top), side="right").astype(jnp.int32)
    grid = items.reshape(top, rows).T
    grid = grid[jax.random.permutation(jax.random.fold_in(own, 1), rows)]
    rotation = jax.random.randint(jax.random.fold_in(own, 2), (rows, 1), 0, top)
    return jnp.take_along_axis(grid, (jnp.arange(top)[None, :] + rotation) % top, axis=1)


def load_shares(count, total, bound, slope, full):
    loads = [(1 << 20) // math.isqrt(grade ** slope) + 1 for grade in range(1, count + 1)]
    largest = bound if full else min(bound, max(-(-total // count), total * loads[0] // sum(loads)))
    least = 1 if total - largest >= count - 1 else 0
    holding, rest = [largest] + [least] * (count - 1), total - largest - least * (count - 1)
    while rest > 0:
        free = [i for i in range(1, count) if holding[i] < largest] or [i for i in range(1, count) if holding[i] < bound]
        mass, left = sum([loads[i] for i in free]), rest
        for i in free:
            addition = min(bound - holding[i], max(1, left * loads[i] // mass), rest)
            holding[i] = holding[i] + addition
            rest = rest - addition
    return np.array(holding)


def centred(rng, shape, width, most, pieces=(), kind=jnp.bfloat16):
    gain = levels(rng, shape, pieces, -0.22, 0.18) if pieces else 1.0
    entries = jax.random.normal(rng, shape, jnp.float32) * width * gain
    return jnp.minimum(jnp.maximum(entries, -most), most).astype(kind)


def noise_with(rng, shape, scale, limit, pieces, heavy, kind=jnp.bfloat16):
    entries = scale * jax.random.normal(rng, shape, jnp.float32)
    if pieces:
        entries = entries * levels(rng, shape, pieces, -0.22, 0.18)
    return jnp.clip(spiked(entries, jax.random.fold_in(rng, 3), *heavy), -limit, limit).astype(kind)


def setup_inputs(seed: int = 0) -> dict:
    key_list = jax.random.split(jax.random.key(seed), 15)
    expert_input = centred(key_list[0], (TOKENS, D), 1.0, 6.0, ((0, 8),))
    cotangent = noise_with(key_list[1], (TOKENS, D), 1.0, 6.0, ((0, 8),), (0, 1, 8, 2.0))
    routes_keys = jax.random.split(jax.random.fold_in(key_list[2], 1), TOKENS // TOK_DEV)
    routes_turns = jax.random.permutation(jax.random.fold_in(key_list[2], 3), TOKENS // TOK_DEV)
    routes = jax.vmap(lambda own, number: assign_block(jax.random.fold_in(key_list[2], 2), own, number, TOK_DEV, EXPERTS, TOP, CAP, 1))(routes_keys, routes_turns).reshape((TOKENS, TOP))
    route_weight = jnp.clip(jnp.exp(math.log(2.5) - 2.5257286 * jax.random.uniform(key_list[3], (TOKENS, TOP), jnp.float32) ** levels(key_list[3], (TOKENS, TOP), ((0, 8),), -0.2, 0.2)), 0.2, 2.5)
    expert_gate = centred(key_list[4], (EXPERTS, D, FF), D ** -0.5, 0.125, ((0, 8), (2, 4)))
    expert_up = centred(key_list[5], (EXPERTS, D, FF), D ** -0.5, 0.125, ((0, 8), (2, 4)))
    expert_down = centred(key_list[6], (EXPERTS, FF, D), FF ** -0.5, 0.1875, ((0, 8), (1, 4)))
    conv_out = draw_conv_out(jax.random.fold_in(key_list[14], 71), 0)
    conv_value = centred(key_list[8], (TOKENS, CW), 1.0, 6.0, ((0, 8), (1, 4)))
    conv_gate = centred(key_list[9], (TOKENS, CW), 1.0, 6.0, ((0, 8), (1, 4)))
    conv_taps = centred(key_list[10], (KW, CW), KW ** -0.5, 1.0, ((1, 4),), jnp.float32)
    norm_gain = jnp.clip(1.0 + 0.18 * jax.random.normal(key_list[11], (CW,), jnp.float32), 0.1, 1.9)
    norm_bias = centred(key_list[12], (CW,), 0.5, 3.0, ((0, 4),), jnp.float32)
    out_weight = centred(key_list[13], (CW, D), CW ** -0.5, 0.1875, ((0, 4),))
    return {"expert_input": expert_input, "cotangent": cotangent, "routes": routes, "route_weight": route_weight, "expert_gate": expert_gate, "expert_up": expert_up, "expert_down": expert_down, "conv_out": conv_out, "conv_value": conv_value, "conv_gate": conv_gate, "conv_taps": conv_taps, "norm_gain": norm_gain, "norm_bias": norm_bias, "out_weight": out_weight}


norm_eps = 1e-06

def build_slots(block_routes):
    assigns = block_routes.shape[0] * block_routes.shape[1]
    flat_routes = block_routes.reshape(assigns)
    onehot = (flat_routes[:, None] == jnp.arange(EXPERTS, dtype=jnp.int32)[None, :]).astype(jnp.int32)
    slot_rank = lax.optimization_barrier(jnp.sum((jnp.cumsum(onehot, axis=0) - onehot) * onehot, axis=1))
    target = flat_routes * CAP + slot_rank
    return jnp.full((EXPERTS * CAP,), assigns, jnp.int32).at[target].set(jnp.arange(assigns, dtype=jnp.int32))

def reference(expert_input, cotangent, routes, route_weight, expert_gate, expert_up, expert_down, conv_out, conv_value, conv_gate, conv_taps, norm_gain, norm_bias, out_weight):
    block_assigns = TOK_DEV * TOP
    slot_sets = jax.vmap(build_slots)(routes.reshape(N_SP, TOK_DEV, TOP))
    offsets = (jnp.arange(N_SP, dtype=jnp.int32) * block_assigns)[:, None]
    global_ids = jnp.where(slot_sets == block_assigns, TOKENS * TOP, slot_sets + offsets).astype(jnp.int32)
    expert_ids = global_ids.reshape(N_SP, EXPERTS, CAP).transpose(1, 0, 2).reshape(EXPERTS, N_SP * CAP)
    scaled = (cotangent.astype(jnp.float32)[:, None, :] * route_weight[:, :, None]).astype(jnp.bfloat16)
    padded_cot = jnp.concatenate([scaled.reshape(TOKENS * TOP, D), jnp.zeros((1, D), jnp.bfloat16)], axis=0)
    padded_in = jnp.concatenate([expert_input, jnp.zeros((1, D), jnp.bfloat16)], axis=0)

    def expert_step(routed, inputs):
        slot_ids, w_gate, w_up, w_down = inputs
        tokens_of = slot_ids // TOP
        slot_rows = padded_in[tokens_of]
        slot_cots = padded_cot[slot_ids]
        pre_gate = jnp.dot(slot_rows, w_gate, preferred_element_type=jnp.float32)
        pre_up = jnp.dot(slot_rows, w_up, preferred_element_type=jnp.float32)
        gate_sig = jax.nn.sigmoid(pre_gate)
        gate_act = pre_gate * gate_sig
        hidden = (gate_act * pre_up).astype(jnp.bfloat16)
        hidden_grad = jnp.dot(slot_cots, w_down.T, preferred_element_type=jnp.float32)
        down_part = jnp.dot(hidden.T, slot_cots, preferred_element_type=jnp.float32)
        gate_pre = (hidden_grad * pre_up * gate_sig * (1.0 + pre_gate * (1.0 - gate_sig))).astype(jnp.bfloat16)
        up_pre = (hidden_grad * gate_act).astype(jnp.bfloat16)
        gate_part = jnp.dot(slot_rows.T, gate_pre, preferred_element_type=jnp.float32)
        up_part = jnp.dot(slot_rows.T, up_pre, preferred_element_type=jnp.float32)
        slot_grad = jnp.zeros((slot_rows.shape[0], D), jnp.float32)
        for group_idx in range(N_TP):
            group_lo = group_idx * FGROUP
            group_hi = group_lo + FGROUP
            group_part = jnp.dot(gate_pre[:, group_lo:group_hi], w_gate[:, group_lo:group_hi].T, preferred_element_type=jnp.float32)
            group_part = group_part + jnp.dot(up_pre[:, group_lo:group_hi], w_up[:, group_lo:group_hi].T, preferred_element_type=jnp.float32)
            slot_grad = slot_grad + lax.optimization_barrier(group_part.astype(jnp.bfloat16)).astype(jnp.float32)
        rounded = lax.optimization_barrier(slot_grad.astype(jnp.bfloat16)).astype(jnp.float32)
        routed = routed.at[tokens_of].add(rounded)
        return (routed, (gate_part, up_part, down_part))
    routed, weight_grads = lax.scan(expert_step, jnp.zeros((TOKENS + 1, D), jnp.float32), (expert_ids, expert_gate, expert_up, expert_down))
    gate_grad, up_grad, down_grad = weight_grads
    resid_grad = (cotangent.astype(jnp.float32) + routed[:TOKENS]).astype(jnp.bfloat16)
    mix_grad = jnp.dot(resid_grad, out_weight.T, preferred_element_type=jnp.float32)
    conv_vals = conv_out.astype(jnp.float32)
    row_mean = lax.optimization_barrier(jnp.mean(conv_vals, axis=1, keepdims=True))
    row_var = lax.optimization_barrier(jnp.mean((conv_vals - row_mean) ** 2, axis=1, keepdims=True))
    row_rstd = lax.rsqrt(row_var + norm_eps)
    normed = (conv_vals - row_mean) * row_rstd
    norm_pre = normed * norm_gain[None, :] + norm_bias[None, :]
    norm_sig = jax.nn.sigmoid(norm_pre)
    conv_act = (norm_pre * norm_sig).astype(jnp.bfloat16)
    out_weight_grad = jnp.dot(conv_act.T, resid_grad, preferred_element_type=jnp.float32)
    norm_grad = mix_grad * norm_sig * (1.0 + norm_pre * (1.0 - norm_sig)) * norm_gain[None, :]
    grad_mean = lax.optimization_barrier(jnp.mean(norm_grad, axis=1, keepdims=True))
    grad_dot = lax.optimization_barrier(jnp.mean(norm_grad * normed, axis=1, keepdims=True))
    conv_grad = row_rstd * (norm_grad - grad_mean - normed * grad_dot)
    extended = jnp.concatenate([conv_grad, jnp.zeros((KW - 1, CW), jnp.float32)], axis=0)
    glu_grad = jnp.zeros((TOKENS, CW), jnp.float32)
    for lag_index in range(KW):
        begin = KW - 1 - lag_index
        glu_grad = glu_grad + conv_taps[lag_index][None, :] * extended[begin:begin + TOKENS]
    gate_sig = jax.nn.sigmoid(conv_gate.astype(jnp.float32))
    value_grad = (glu_grad * gate_sig).astype(jnp.bfloat16)
    gate_in_grad = (glu_grad * conv_value.astype(jnp.float32) * gate_sig * (1.0 - gate_sig)).astype(jnp.bfloat16)
    return (gate_grad, up_grad, down_grad, resid_grad, out_weight_grad, value_grad, gate_in_grad)
```

```python
import functools

import jax
import jax.numpy as jnp
from jax import lax
from jax.experimental import pallas as pl
from jax.experimental.pallas import tpu as pltpu
from jax.sharding import PartitionSpec as P

norm_eps = 1e-06
f32 = jnp.float32
bf16 = jnp.bfloat16


def mm(a, b, ca, cb):
    return lax.dot_general(a, b, (((ca,), (cb,)), ((), ())), preferred_element_type=f32)


def exact_mm(a, b, ca, cb):
    return lax.dot_general(
        a, b, (((ca,), (cb,)), ((), ())), preferred_element_type=f32, precision=lax.Precision.HIGHEST
    )


def params():
    return pltpu.CompilerParams(vmem_limit_bytes=58 * 1024 * 1024)


def tp_swap(value, dist):
    count = lax.axis_size("tp")
    return lax.ppermute(value, "tp", [(i, i ^ dist) for i in range(count)])


def tp_pieces(own):
    near = tp_swap(own, 1)
    far = tp_swap(own, 2)
    return (own, near, far, tp_swap(far, 1))


def passed_along(value, axis, steps):
    count = lax.axis_size(axis)
    leading, last = (max(0, -steps), min(count, count - steps))
    return lax.ppermute(value, axis, [(source, source + steps) for source in range(leading, last)])


def dispatch_body(tp_ref, routes_ref, weight_ref, input_ref, cot_ref, rows_ref, cots_ref):
    experts, capacity, _ = rows_ref.shape
    tokens = routes_ref.shape[1]
    top = routes_ref.shape[0]
    expert_id = lax.broadcasted_iota(jnp.int32, (experts, tokens), 0)
    named = jnp.zeros((experts, tokens), f32)
    weights = jnp.zeros((experts, tokens), f32)
    for k in range(top):
        hit = routes_ref[k : k + 1, :] == expert_id
        named = jnp.where(hit, 1.0, named)
        weights = jnp.where(hit, weight_ref[k : k + 1, :], weights)
    before = lax.broadcasted_iota(jnp.int32, (tokens, tokens), 0) < lax.broadcasted_iota(
        jnp.int32, (tokens, tokens), 1
    )
    rank = mm(named.astype(bf16), jnp.where(before, 1.0, 0.0).astype(bf16), 1, 0)
    key = jnp.where(named > 0.5, rank, -1.0).astype(jnp.int32)
    slot = lax.broadcasted_iota(jnp.int32, (capacity, tokens), 0)
    for e in range(experts):
        pick = slot == key[e : e + 1, :]
        chosen = jnp.where(pick, 1.0, 0.0).astype(bf16)
        slot_weight = jnp.sum(jnp.where(pick, weights[e : e + 1, :], 0.0), axis=1, keepdims=True)
        rows_ref[e] = mm(chosen, input_ref[...], 1, 0).astype(bf16)
        cots_ref[e] = (mm(chosen, cot_ref[...], 1, 0) * slot_weight).astype(bf16)


def dispatch(tp_idx, routes_t, weight_t, expert_input, cotangent, experts, capacity, share):
    tokens = expert_input.shape[0]
    whole = lambda *shape: pl.BlockSpec(shape, lambda i, tp: (0,) * len(shape))
    quarter = pl.BlockSpec((tokens, share), lambda i, tp: (0, tp[0]))
    out = jax.ShapeDtypeStruct((experts, capacity, share), bf16)
    return pl.pallas_call(
        dispatch_body,
        grid_spec=pltpu.PrefetchScalarGridSpec(
            num_scalar_prefetch=1,
            grid=(1,),
            in_specs=[whole(*routes_t.shape), whole(*weight_t.shape), quarter, quarter],
            out_specs=[whole(*out.shape)] * 2,
        ),
        out_shape=[out, out],
        compiler_params=params(),
        name="dispatch",
    )(tp_idx, routes_t, weight_t, expert_input, cotangent)


def pre_body(tp_ref, p0, p1, p2, p3, wg_ref, wu_ref, gate_ref, up_ref):
    share = p0.shape[1]
    gate = None
    for j, piece in enumerate((p0, p1, p2, p3)):
        at = pl.ds(pl.multiple_of((tp_ref[0] ^ j) * share, share), share)
        rows = piece[...]
        g = mm(rows, wg_ref[at, :], 1, 0)
        u = mm(rows, wu_ref[at, :], 1, 0)
        gate, up = (g, u) if gate is None else (gate + g, up + u)
    gate_ref[...] = gate
    up_ref[...] = up


def row_block(rows):
    for block in (288, 192, 96):
        if rows % block == 0:
            return block
    return rows


def pre_acts(tp_idx, pieces, w_gate, w_up):
    rows, share = pieces[0].shape
    width = w_gate.shape[1]
    block = row_block(rows)
    row_spec = pl.BlockSpec((block, share), lambda i, tp: (i, 0))
    w_spec = pl.BlockSpec(w_gate.shape, lambda i, tp: (0, 0))
    out_spec = pl.BlockSpec((block, width), lambda i, tp: (i, 0))
    out = jax.ShapeDtypeStruct((rows, width), f32)
    return pl.pallas_call(
        pre_body,
        grid_spec=pltpu.PrefetchScalarGridSpec(
            num_scalar_prefetch=1,
            grid=(rows // block,),
            in_specs=[row_spec] * 4 + [w_spec] * 2,
            out_specs=[out_spec] * 2,
        ),
        out_shape=[out, out],
        compiler_params=params(),
        name="pre_acts",
    )(tp_idx, *pieces, w_gate, w_up)


def hidden_body(tp_ref, p0, p1, p2, p3, wd_ref, gate_ref, up_ref, hid_ref, gp_ref, up_out_ref):
    share = p0.shape[1]
    grad = None
    for j, piece in enumerate((p0, p1, p2, p3)):
        at = pl.ds(pl.multiple_of((tp_ref[0] ^ j) * share, share), share)
        h = mm(piece[...], wd_ref[:, at], 1, 1)
        grad = h if grad is None else grad + h
    gate = gate_ref[...]
    up = up_ref[...]
    sig = jax.nn.sigmoid(gate)
    act = gate * sig
    hid_ref[...] = (act * up).astype(bf16)
    gp_ref[...] = (grad * up * sig * (1.0 + gate * (1.0 - sig))).astype(bf16)
    up_out_ref[...] = (grad * act).astype(bf16)


def hidden_grads(tp_idx, pieces, w_down, gate, up):
    rows, share = pieces[0].shape
    width = w_down.shape[0]
    block = row_block(rows)
    row_spec = pl.BlockSpec((block, share), lambda i, tp: (i, 0))
    w_spec = pl.BlockSpec(w_down.shape, lambda i, tp: (0, 0))
    mid = pl.BlockSpec((block, width), lambda i, tp: (i, 0))
    out = jax.ShapeDtypeStruct((rows, width), bf16)
    return pl.pallas_call(
        hidden_body,
        grid_spec=pltpu.PrefetchScalarGridSpec(
            num_scalar_prefetch=1,
            grid=(rows // block,),
            in_specs=[row_spec] * 4 + [w_spec] + [mid] * 2,
            out_specs=[mid] * 3,
        ),
        out_shape=[out] * 3,
        compiler_params=params(),
        name="hidden_grads",
    )(tp_idx, *pieces, w_down, gate, up)


def slot_body(tp_ref, gp_ref, up_ref, wg_ref, wu_ref, *outs, cols, lo):
    share = wg_ref.shape[0] // 4
    gp = gp_ref[...]
    up = up_ref[...]
    for j, out in enumerate(outs):
        at = pl.ds(pl.multiple_of((tp_ref[0] ^ j) * share + lo, cols), cols)
        out[...] = (mm(gp, wg_ref[at, :], 1, 1) + mm(up, wu_ref[at, :], 1, 1)).astype(bf16)


def slot_grads(tp_idx, gate_pre, up_pre, w_gate, w_up, cols, lo):
    rows, width = gate_pre.shape
    block = row_block(rows)
    mid = pl.BlockSpec((block, width), lambda i, tp: (i, 0))
    w_spec = pl.BlockSpec(w_gate.shape, lambda i, tp: (0, 0))
    out_spec = pl.BlockSpec((block, cols), lambda i, tp: (i, 0))
    out = jax.ShapeDtypeStruct((rows, cols), bf16)
    return pl.pallas_call(
        functools.partial(slot_body, cols=cols, lo=lo),
        grid_spec=pltpu.PrefetchScalarGridSpec(
            num_scalar_prefetch=1,
            grid=(rows // block,),
            in_specs=[mid] * 2 + [w_spec] * 2,
            out_specs=[out_spec] * 4,
        ),
        out_shape=[out] * 4,
        compiler_params=params(),
        name="slot_grads",
    )(tp_idx, gate_pre, up_pre, w_gate, w_up)


def wide_body(tp_ref, p0, p1, p2, p3, gp_ref, up_ref, gg_ref, ug_ref):
    share = p0.shape[1]
    gp = gp_ref[...]
    up = up_ref[...]
    for j, piece in enumerate((p0, p1, p2, p3)):
        at = pl.ds(pl.multiple_of((tp_ref[0] ^ j) * share, share), share)
        rows = piece[...]
        gg_ref[at, :] = mm(rows, gp, 0, 0)
        ug_ref[at, :] = mm(rows, up, 0, 0)


def down_body(tp_ref, p0, p1, p2, p3, hid_ref, dg_ref):
    share = p0.shape[1]
    hid = hid_ref[...]
    for j, piece in enumerate((p0, p1, p2, p3)):
        at = pl.ds(pl.multiple_of((tp_ref[0] ^ j) * share, share), share)
        dg_ref[:, at] = mm(hid, piece[...], 0, 0)


def grads_call(body, name, tp_idx, args, out_shapes):
    spec = lambda shape: pl.BlockSpec(shape, lambda i, tp: (0,) * len(shape))
    return pl.pallas_call(
        body,
        grid_spec=pltpu.PrefetchScalarGridSpec(
            num_scalar_prefetch=1,
            grid=(1,),
            in_specs=[spec(a.shape) for a in args],
            out_specs=[spec(s) for s, _ in out_shapes],
        ),
        out_shape=[jax.ShapeDtypeStruct(s, d) for s, d in out_shapes],
        compiler_params=params(),
        name=name,
    )(tp_idx, *args)


def combine_body(tp_ref, routes_ref, cot_ref, *refs):
    backs, out_ref = refs[:-1], refs[-1]
    experts, capacity, cols = backs[0].shape
    tokens, top = routes_ref.shape
    expert_id = lax.broadcasted_iota(jnp.int32, (tokens, experts), 1)
    named = jnp.zeros((tokens, experts), f32)
    for k in range(top):
        named = jnp.where(routes_ref[:, k : k + 1] == expert_id, 1.0, named)
    before = lax.broadcasted_iota(jnp.int32, (tokens, tokens), 1) < lax.broadcasted_iota(
        jnp.int32, (tokens, tokens), 0
    )
    rank = mm(jnp.where(before, 1.0, 0.0).astype(bf16), named.astype(bf16), 1, 0)
    key = jnp.where(named > 0.5, rank, -1.0).astype(jnp.int32)
    slot = lax.broadcasted_iota(jnp.int32, (tokens, capacity), 1)
    totals = [cot_ref[:, b * cols : (b + 1) * cols].astype(f32) for b in range(len(backs))]
    sums = [None] * len(backs)
    for e in range(experts):
        chosen = jnp.where(slot == key[:, e : e + 1], 1.0, 0.0).astype(bf16)
        for b, back in enumerate(backs):
            part = mm(chosen, back[e], 1, 0)
            sums[b] = part if sums[b] is None else sums[b] + part
    for b in range(len(backs)):
        out_ref[:, b * cols : (b + 1) * cols] = (totals[b] + sums[b]).astype(bf16)


def combine(tp_idx, routes, cotangent, backs, share):
    tokens = routes.shape[0]
    whole = lambda shape: pl.BlockSpec(shape, lambda i, tp: (0,) * len(shape))
    return pl.pallas_call(
        combine_body,
        grid_spec=pltpu.PrefetchScalarGridSpec(
            num_scalar_prefetch=1,
            grid=(1,),
            in_specs=[whole(routes.shape), pl.BlockSpec((tokens, share), lambda i, tp: (0, tp[0]))]
            + [whole(b.shape) for b in backs],
            out_specs=whole((tokens, share)),
        ),
        out_shape=jax.ShapeDtypeStruct((tokens, share), bf16),
        compiler_params=params(),
        name="combine",
    )(tp_idx, routes, cotangent, *backs)


def norm_parts(conv_ref, mean_ref, gain_ref, bias_ref):
    normed = (conv_ref[...].astype(f32) - mean_ref[:, 0:1]) * mean_ref[:, 1:2]
    pre = normed * gain_ref[...] + bias_ref[...]
    sig = jax.nn.sigmoid(pre)
    return normed, pre, sig


def mix_body(tp_ref, p0, p1, p2, p3, w_ref, conv_ref, mean_ref, gain_ref, bias_ref, resid_ref, ng_ref, sums_ref):
    share = p0.shape[1]
    mix = None
    for j, piece in enumerate((p0, p1, p2, p3)):
        at = pl.ds(pl.multiple_of((tp_ref[0] ^ j) * share, share), share)
        rows = piece[...]
        resid_ref[:, at] = rows
        part = mm(rows, w_ref[:, at], 1, 1)
        mix = part if mix is None else mix + part
    normed, pre, sig = norm_parts(conv_ref, mean_ref, gain_ref, bias_ref)
    grad = mix * sig * (1.0 + pre * (1.0 - sig)) * gain_ref[...]
    ng_ref[...] = grad
    ones = jnp.ones((8, grad.shape[1]), f32)
    total = exact_mm(ones, grad, 1, 1)
    dot = exact_mm(ones, grad * normed, 1, 1)
    row = lax.broadcasted_iota(jnp.int32, total.shape, 0)
    sums_ref[...] = jnp.where(row == 0, total, dot)


def owg_body(tp_ref, p0, p1, p2, p3, conv_ref, mean_ref, gain_ref, bias_ref, out_ref):
    blocks, _, cols = out_ref.shape
    per = blocks // 4
    normed, pre, sig = norm_parts(conv_ref, mean_ref, gain_ref, bias_ref)
    act = (pre * sig).astype(bf16)
    for j, piece in enumerate((p0, p1, p2, p3)):
        part = mm(act, piece[...], 0, 0).astype(bf16)
        for b in range(per):
            out_ref[(tp_ref[0] ^ j) * per + b] = part[:, b * cols : (b + 1) * cols]


def on_device(
    expert_input,
    cotangent,
    routes,
    route_weight,
    expert_gate,
    expert_up,
    expert_down,
    conv_out,
    conv_value,
    conv_gate,
    conv_taps,
    norm_gain,
    norm_bias,
    out_weight,
):
    sp_count = lax.axis_size("sp")
    tp_count = lax.axis_size("tp")
    assert tp_count == 4 and expert_gate.shape[0] == 1
    tok_rows, model_width = expert_input.shape
    share = model_width // tp_count
    top_count = routes.shape[1]
    experts = sp_count
    capacity = 3 * top_count * tok_rows // (2 * experts)
    slots = sp_count * capacity
    w_gate, w_up, w_down = expert_gate[0], expert_up[0], expert_down[0]
    width = w_gate.shape[1]
    chan = conv_out.shape[1]
    channels = chan * tp_count
    tp_idx = lax.axis_index("tp").astype(jnp.int32).reshape(1)

    send_rows, send_cots = dispatch(
        tp_idx, routes.T, route_weight.T, expert_input, cotangent, experts, capacity, share
    )
    got_rows = lax.all_to_all(send_rows, "sp", split_axis=0, concat_axis=0, tiled=True)
    got_cots = lax.all_to_all(send_cots, "sp", split_axis=0, concat_axis=0, tiled=True)

    conv_vals = conv_out.astype(f32)
    own_mean = jnp.mean(conv_vals, axis=1)
    own_m2 = jnp.sum((conv_vals - own_mean[:, None]) ** 2, axis=1)
    own_stat = jnp.stack([own_mean, own_m2])
    stats = [own_stat] + [tp_swap(own_stat, d) for d in (1, 2, 3)]
    row_mean = sum(s[0] for s in stats) / tp_count
    row_m2 = sum(s[1] + chan * (s[0] - row_mean) ** 2 for s in stats)
    row_rstd = lax.rsqrt(row_m2 / channels + norm_eps)
    mean_rstd = jnp.stack([row_mean, row_rstd], axis=1)

    row_pieces = tp_pieces(got_rows.reshape(slots, share))
    cot_pieces = tp_pieces(got_cots.reshape(slots, share))
    pre_gate, pre_up = pre_acts(tp_idx, row_pieces, w_gate, w_up)
    hidden, gate_pre, up_pre = hidden_grads(tp_idx, cot_pieces, w_down, pre_gate, pre_up)

    chunks = 2
    cols = share // chunks
    backs = []
    for c in range(chunks):
        o0, o1, o2, o3 = slot_grads(tp_idx, gate_pre, up_pre, w_gate, w_up, cols, c * cols)
        r3 = tp_swap(o3, 1)
        r1 = tp_swap(o1, 1)
        s2 = (o2.astype(f32) + r3.astype(f32)).astype(bf16)
        r2 = tp_swap(s2, 2)
        total = (o0.astype(f32) + r1.astype(f32) + r2.astype(f32)).astype(bf16)
        backs.append(
            lax.all_to_all(
                total.reshape(sp_count, capacity, cols), "sp", split_axis=0, concat_axis=0, tiled=True
            )
        )
    gate_grad, up_grad = grads_call(
        wide_body,
        "wide_grads",
        tp_idx,
        (*row_pieces, gate_pre, up_pre),
        [((model_width, width), f32)] * 2,
    )
    (down_grad,) = grads_call(
        down_body, "down_grads", tp_idx, (*cot_pieces, hidden), [((width, model_width), f32)]
    )

    resid_part = combine(tp_idx, routes, cotangent, backs, share)
    resid_pieces = tp_pieces(resid_part)
    gain_row, bias_row = norm_gain[None, :], norm_bias[None, :]
    norm_args = (conv_out, mean_rstd, gain_row, bias_row)
    resid_grad, norm_grad, own_sums = grads_call(
        mix_body,
        "mix_grads",
        tp_idx,
        (*resid_pieces, out_weight, *norm_args),
        [((tok_rows, model_width), bf16), ((tok_rows, chan), f32), ((8, tok_rows), f32)],
    )
    own_sums = own_sums[:2]
    all_sums = own_sums + tp_swap(own_sums, 1) + tp_swap(own_sums, 2) + tp_swap(own_sums, 3)
    (projected,) = grads_call(
        owg_body,
        "owg",
        tp_idx,
        (*resid_pieces, *norm_args),
        [((sp_count, chan, model_width // sp_count), bf16)],
    )
    arrived = lax.all_to_all(projected, "sp", split_axis=0, concat_axis=0, tiled=True)
    out_weight_grad = jnp.sum(arrived.astype(f32), axis=0)

    normed = (conv_vals - row_mean[:, None]) * row_rstd[:, None]
    conv_grad = row_rstd[:, None] * (
        norm_grad
        - (all_sums[0] / channels)[:, None]
        - normed * (all_sums[1] / channels)[:, None]
    )
    taps_count = conv_taps.shape[0]
    next_rows = passed_along(conv_grad[: taps_count - 1], "sp", -1)
    extended = jnp.concatenate([conv_grad, next_rows], axis=0)
    glu_grad = jnp.zeros_like(conv_grad)
    for lag_index in range(taps_count):
        begin = taps_count - 1 - lag_index
        glu_grad = glu_grad + conv_taps[lag_index][None, :] * extended[begin : begin + tok_rows]
    gate_sig_in = jax.nn.sigmoid(conv_gate.astype(f32))
    value_grad = (glu_grad * gate_sig_in).astype(bf16)
    gate_in_grad = (
        glu_grad * conv_value.astype(f32) * gate_sig_in * (1.0 - gate_sig_in)
    ).astype(bf16)
    return (
        gate_grad[None],
        up_grad[None],
        down_grad[None],
        resid_grad,
        out_weight_grad,
        value_grad,
        gate_in_grad,
    )


def solution(mesh):
    return jax.shard_map(
        on_device,
        mesh=mesh,
        in_specs=(
            P("sp", None),
            P("sp", None),
            P("sp", None),
            P("sp", None),
            P("sp", None, "tp"),
            P("sp", None, "tp"),
            P("sp", "tp", None),
            P("sp", "tp"),
            P("sp", "tp"),
            P("sp", "tp"),
            P(None, "tp"),
            P("tp"),
            P("tp"),
            P("tp", None),
        ),
        out_specs=(
            P("sp", None, "tp"),
            P("sp", None, "tp"),
            P("sp", "tp", None),
            P("sp", None),
            P("tp", "sp"),
            P("sp", "tp"),
            P("sp", "tp"),
        ),
        check_vma=False,
    )
```

```python
import functools
import math

import jax
import jax.numpy as jnp
from jax import lax
from jax.experimental import pallas as pl
from jax.experimental.pallas import tpu as pltpu
from jax.sharding import PartitionSpec as P


norm_eps = 1e-06
f32 = jnp.float32
bf16 = jnp.bfloat16


def mm(a, b, ca, cb):
    return lax.dot_general(a, b, (((ca,), (cb,)), ((), ())), preferred_element_type=f32)


def exact_mm(a, b, ca, cb):
    return lax.dot_general(
        a, b, (((ca,), (cb,)), ((), ())), preferred_element_type=f32, precision=lax.Precision.HIGHEST
    )


def params(blocks, copies):
    if copies == 0:
        return pltpu.CompilerParams(vmem_limit_bytes=56 * 1024 * 1024)
    need = sum(math.prod(shape) * jnp.dtype(kind).itemsize for shape, kind in blocks)
    return pltpu.CompilerParams(vmem_limit_bytes=copies * need + 8 * 1024 * 1024)


def tp_swap(value, dist):
    count = lax.axis_size("tp")
    return lax.ppermute(value, "tp", [(i, i ^ dist) for i in range(count)])


def tp_pieces(own):
    far = tp_swap(own, 2)
    return (own, tp_swap(own, 1), far, tp_swap(far, 1))


def passed_along(value, axis, steps):
    count = lax.axis_size(axis)
    leading, last = (max(0, -steps), min(count, count - steps))
    return lax.ppermute(value, axis, [(source, source + steps) for source in range(leading, last)])


def dispatch_body(at_ref, routes_ref, weight_ref, source_ref, *outs, cots):
    experts, capacity = len(outs), outs[0].shape[0]
    top, tokens = routes_ref.shape
    expert_id = lax.broadcasted_iota(jnp.int32, (experts, tokens), 0)
    named = jnp.zeros((experts, tokens), f32)
    weights = jnp.zeros((experts, tokens), f32)
    for k in range(top):
        hit = (routes_ref[k : k + 1, :] ^ at_ref[1]) == expert_id
        named = jnp.where(hit, 1.0, named)
        weights = jnp.where(hit, weight_ref[k : k + 1, :], weights)
    before = lax.broadcasted_iota(jnp.int32, (tokens, tokens), 0) < lax.broadcasted_iota(
        jnp.int32, (tokens, tokens), 1
    )
    rank = mm(named.astype(bf16), jnp.where(before, 1.0, 0.0).astype(bf16), 1, 0)
    key = jnp.where(named > 0.5, rank, -1.0).astype(jnp.int32)
    slot = lax.broadcasted_iota(jnp.int32, (capacity, tokens), 0)
    for e in range(experts):
        pick = slot == key[e : e + 1, :]
        rows = mm(jnp.where(pick, 1.0, 0.0).astype(bf16), source_ref[...], 1, 0)
        if cots:
            rows = rows * jnp.sum(jnp.where(pick, weights[e : e + 1, :], 0.0), axis=1, keepdims=True)
        outs[e][...] = rows.astype(bf16)


def whole_spec(shape):
    return pl.BlockSpec(shape, lambda i, at: (0,) * len(shape))


def quarter_spec(tokens, share):
    return pl.BlockSpec((tokens, share), lambda i, at: (0, at[0]))


def call(body, at, args, outs, in_specs=None, out_specs=None, steps=1, keep=True):
    in_specs = in_specs or [whole_spec(a.shape) for a in args]
    out_specs = out_specs or [whole_spec(s) for s, _ in outs]
    blocks = [(spec.block_shape, a.dtype) for spec, a in zip(in_specs, args)]
    blocks += [(spec.block_shape, kind) for spec, (_, kind) in zip(out_specs, outs)]
    return pl.pallas_call(
        body,
        grid_spec=pltpu.PrefetchScalarGridSpec(
            num_scalar_prefetch=1, grid=(steps,), in_specs=in_specs, out_specs=out_specs
        ),
        out_shape=[jax.ShapeDtypeStruct(s, d) for s, d in outs],
        compiler_params=params(blocks, keep * min(steps, 2)),
    )(at, *args)


def dispatch(at, routes_t, weight_t, source, experts, capacity, share, cots):
    outs = [((capacity, share), bf16)] * experts
    return call(
        functools.partial(dispatch_body, cots=cots),
        at,
        (routes_t, weight_t, source),
        outs,
        [whole_spec(routes_t.shape), whole_spec(weight_t.shape), quarter_spec(source.shape[0], share)],
        keep=cots,
    )


def sp_swap(value, dist):
    count = lax.axis_size("sp")
    return lax.ppermute(value, "sp", [(i, i ^ dist) for i in range(count)])


def sp_exchange(blocks):
    got = list(blocks)
    for k in range(1, len(blocks)):
        got[k] = sp_swap(blocks[k], k)
    return got


def sp_all(value):
    return lax.all_to_all(value, "sp", split_axis=0, concat_axis=0, tiled=True)


def join(blocks):
    return jnp.concatenate(blocks, axis=0)


def rows_of(ref):
    return join([ref[i] for i in range(ref.shape[0])])


def store_blocks(ref, value, first=0, count=None):
    capacity = ref.shape[1]
    for i in range(ref.shape[0] if count is None else count):
        ref[first + i] = value[i * capacity : (i + 1) * capacity]


def pre_body(at_ref, p0, p1, p2, p3, wg_ref, wu_ref, gate_ref, up_ref):
    share = p0.shape[2]
    gate, up = 0.0, 0.0
    for j, piece in enumerate((p0, p1, p2, p3)):
        at = pl.ds(pl.multiple_of((at_ref[0] ^ j) * share, share), share)
        rows = rows_of(piece)
        gate = gate + mm(rows, wg_ref[at, :], 1, 0)
        up = up + mm(rows, wu_ref[at, :], 1, 0)
    store_blocks(gate_ref, gate)
    store_blocks(up_ref, up)


def blocked(shape):
    return pl.BlockSpec((2, *shape[1:]), lambda i, at: (i, 0, 0))


def pre_acts(at, pieces, w_gate, w_up):
    count, capacity, _ = pieces[0].shape
    mid = (count, capacity, w_gate.shape[1])
    return call(
        pre_body,
        at,
        (*pieces, w_gate, w_up),
        [(mid, f32)] * 2,
        [blocked(pieces[0].shape)] * 4 + [whole_spec(w_gate.shape)] * 2,
        [blocked(mid)] * 2,
        count // 2,
    )


def hidden_body(at_ref, p0, p1, p2, p3, wd_ref, gate_ref, up_ref, hid_ref, gp_ref, up_out_ref):
    share = p0.shape[2]
    grad = 0.0
    for j, piece in enumerate((p0, p1, p2, p3)):
        at = pl.ds(pl.multiple_of((at_ref[0] ^ j) * share, share), share)
        grad = grad + mm(rows_of(piece), wd_ref[:, at], 1, 1)
    gate = rows_of(gate_ref)
    up = rows_of(up_ref)
    sig = jax.nn.sigmoid(gate)
    act = gate * sig
    store_blocks(hid_ref, (act * up).astype(bf16))
    store_blocks(gp_ref, (grad * up * sig * (1.0 + gate * (1.0 - sig))).astype(bf16))
    store_blocks(up_out_ref, (grad * act).astype(bf16))


def hidden_grads(at, pieces, w_down, gate, up):
    count, capacity, _ = pieces[0].shape
    mid = (count, capacity, w_down.shape[0])
    return call(
        hidden_body,
        at,
        (*pieces, w_down, gate, up),
        [(mid, bf16)] * 3,
        [blocked(pieces[0].shape)] * 4 + [whole_spec(w_down.shape)] + [blocked(mid)] * 2,
        [blocked(mid)] * 3,
        count // 2,
    )


def chunk_parts(share, eighth, chunk, chunks):
    sub = eighth // chunks
    return [(b * eighth + chunk * sub, sub) for b in range(share // eighth)]


def slot_body(at_ref, gp_ref, up_ref, wg_ref, wu_ref, *outs, parts):
    share = wg_ref.shape[0] // 4
    count = gp_ref.shape[0]
    gp = rows_of(gp_ref)
    up = rows_of(up_ref)
    for c, spans in enumerate(parts):
        own_ref, near_ref, far_ref = outs[3 * c : 3 * c + 3]
        for j, out, first in ((3, near_ref, 0), (2, far_ref, 0), (1, near_ref, count), (0, own_ref, 0)):
            base = (at_ref[0] ^ j) * share
            rows = [pl.ds(pl.multiple_of(base + lo, size), size) for lo, size in spans]
            part = mm(gp, join([wg_ref[r, :] for r in rows]), 1, 1)
            part = part + mm(up, join([wu_ref[r, :] for r in rows]), 1, 1)
            store_blocks(out, part.astype(bf16), first, count)


def slot_grads(at, gate_pre, up_pre, w_gate, w_up, parts):
    count, capacity, _ = gate_pre.shape
    cols = sum(size for _, size in parts[0])
    one, two = (count, capacity, cols), (2 * count, capacity, cols)
    return call(
        functools.partial(slot_body, parts=parts),
        at,
        (gate_pre, up_pre, w_gate, w_up),
        [(one, bf16), (two, bf16), (one, bf16)] * len(parts),
    )


def add_body(at_ref, *refs, groups):
    ins, outs = refs[: 3 * groups], refs[3 * groups :]
    for g in range(groups):
        own, near, far = ins[3 * g : 3 * g + 3]
        count = own.shape[0]
        for i in range(count):
            total = own[i].astype(f32) + near[count + i].astype(f32) + far[i].astype(f32)
            outs[g * count + i][...] = total.astype(bf16)


def wide_body(at_ref, *refs, groups):
    pieces, sides, out_ref = refs[: 4 * groups], refs[4 * groups : 5 * groups], refs[5 * groups]
    share = pieces[0].shape[2]
    side = join([rows_of(ref) for ref in sides])
    for j in range(4):
        at = pl.ds(pl.multiple_of((at_ref[0] ^ j) * share, share), share)
        rows = join([rows_of(pieces[4 * g + j]) for g in range(groups)])
        out_ref[at, :] = mm(rows, side, 0, 0)


def down_body(at_ref, *refs, groups):
    pieces, hids, dg_ref = refs[: 4 * groups], refs[4 * groups : 5 * groups], refs[5 * groups]
    share = pieces[0].shape[2]
    hid = join([rows_of(ref) for ref in hids])
    for j in range(4):
        at = pl.ds(pl.multiple_of((at_ref[0] ^ j) * share, share), share)
        rows = join([rows_of(pieces[4 * g + j]) for g in range(groups)])
        dg_ref[:, at] = mm(hid, rows, 0, 0)


def picks_body(at_ref, routes_ref, out_ref):
    experts, tokens, capacity = out_ref.shape
    top = routes_ref.shape[1]
    expert_id = lax.broadcasted_iota(jnp.int32, (tokens, experts), 1)
    named = jnp.zeros((tokens, experts), f32)
    for k in range(top):
        named = jnp.where((routes_ref[:, k : k + 1] ^ at_ref[1]) == expert_id, 1.0, named)
    before = lax.broadcasted_iota(jnp.int32, (tokens, tokens), 1) < lax.broadcasted_iota(
        jnp.int32, (tokens, tokens), 0
    )
    rank = mm(jnp.where(before, 1.0, 0.0).astype(bf16), named.astype(bf16), 1, 0)
    key = jnp.where(named > 0.5, rank, -1.0).astype(jnp.int32)
    slot = lax.broadcasted_iota(jnp.int32, (tokens, capacity), 1)
    for e in range(experts):
        out_ref[e] = jnp.where(slot == key[:, e : e + 1], 1.0, 0.0).astype(bf16)


def combine_body(at_ref, picks_ref, cot_ref, *refs, parts):
    backs, out_ref = refs[:-1], refs[-1]
    total = 0.0
    for e in range(picks_ref.shape[0]):
        total = total + mm(picks_ref[e], backs[e][...], 1, 0)
    cot = jnp.concatenate([cot_ref[:, lo : lo + size] for lo, size in parts], axis=1)
    out_ref[...] = (cot.astype(f32) + total).astype(bf16)


def combine(at, picks, cotangent, back, parts, share):
    tokens = cotangent.shape[0]
    (out,) = call(
        functools.partial(combine_body, parts=parts),
        at,
        (picks, cotangent, *back),
        [((tokens, back[0].shape[-1]), bf16)],
        [whole_spec(picks.shape), quarter_spec(tokens, share)] + [whole_spec(b.shape) for b in back],
    )
    return out


def stats_body(at_ref, conv_ref, out_ref):
    vals = conv_ref[...].astype(f32)
    mean = jnp.mean(vals, axis=1, keepdims=True)
    ones = jnp.ones((2, vals.shape[1]), f32)
    means = exact_mm(ones, vals, 1, 1) * (1.0 / vals.shape[1])
    squares = exact_mm(ones, (vals - mean) ** 2, 1, 1)
    row = lax.broadcasted_iota(jnp.int32, means.shape, 0)
    out_ref[...] = jnp.where(row == 0, means, squares)


def moments_body(at_ref, *refs, chan):
    stats, out_ref = [ref[...] for ref in refs[:-1]], refs[-1]
    count = len(stats)
    mean = sum(s[0:1] for s in stats) / count
    m2 = sum(s[1:2] + chan * (s[0:1] - mean) ** 2 for s in stats)
    rstd = lax.rsqrt(m2 / (count * chan) + norm_eps)
    row = lax.broadcasted_iota(jnp.int32, (2, mean.shape[1]), 0)
    both = jnp.where(row == 0, mean, rstd)
    out_ref[...] = exact_mm(both, jnp.eye(2, dtype=f32), 0, 0)


def norm_parts(conv_ref, mean_ref, gain_ref, bias_ref):
    normed = (conv_ref[...].astype(f32) - mean_ref[:, 0:1]) * mean_ref[:, 1:2]
    pre = normed * gain_ref[...] + bias_ref[...]
    sig = jax.nn.sigmoid(pre)
    return normed, pre, sig


def mix_body(at_ref, *refs, parts):
    pieces, refs = refs[: 4 * len(parts)], refs[4 * len(parts) :]
    w_ref, conv_ref, mean_ref, gain_ref, bias_ref, resid_ref, ng_ref, sums_ref = refs
    share = resid_ref.shape[1] // 4
    for c, spans in enumerate(parts):
        for j in range(4):
            base = (at_ref[0] ^ j) * share
            rows = pieces[4 * c + j]
            if len(parts) == 1:
                resid_ref[:, pl.ds(pl.multiple_of(base, share), share)] = rows[...]
                continue
            for b, (lo, size) in enumerate(spans):
                at = pl.ds(pl.multiple_of(base + lo, size), size)
                resid_ref[:, at] = rows[:, b * size : (b + 1) * size]
    mix = mm(resid_ref[...], w_ref[...], 1, 1)
    normed, pre, sig = norm_parts(conv_ref, mean_ref, gain_ref, bias_ref)
    grad = mix * sig * (1.0 + pre * (1.0 - sig)) * gain_ref[...]
    ng_ref[...] = grad
    ones = jnp.ones((2, grad.shape[1]), f32)
    total = exact_mm(ones, grad, 1, 1)
    dot = exact_mm(ones, grad * normed, 1, 1)
    row = lax.broadcasted_iota(jnp.int32, total.shape, 0)
    sums_ref[...] = jnp.where(row == 0, total, dot)


def gates_body(at_ref, value_ref, gate_ref, a_ref, b_ref):
    sig = jax.nn.sigmoid(gate_ref[...].astype(f32))
    a_ref[...] = sig
    b_ref[...] = value_ref[...].astype(f32) * sig * (1.0 - sig)


def owg_body(at_ref, p0, p1, p2, p3, conv_ref, mean_ref, gain_ref, bias_ref, out_ref):
    blocks, _, cols = out_ref.shape
    per = blocks // 4
    _, pre, sig = norm_parts(conv_ref, mean_ref, gain_ref, bias_ref)
    act = (pre * sig).astype(bf16)
    for j, piece in enumerate((p0, p1, p2, p3)):
        part = mm(act, piece[...], 0, 0).astype(bf16)
        for b in range(per):
            out_ref[(at_ref[0] ^ j) * per + b] = part[:, b * cols : (b + 1) * cols]


def on_device(
    expert_input,
    cotangent,
    routes,
    route_weight,
    expert_gate,
    expert_up,
    expert_down,
    conv_out,
    conv_value,
    conv_gate,
    conv_taps,
    norm_gain,
    norm_bias,
    out_weight,
):
    sp_count = lax.axis_size("sp")
    tp_count = lax.axis_size("tp")
    assert tp_count == 4 and expert_gate.shape[0] == 1
    tok_rows, model_width = expert_input.shape
    share = model_width // tp_count
    eighth = model_width // sp_count
    top_count = routes.shape[1]
    experts = sp_count
    capacity = 3 * top_count * tok_rows // (2 * experts)
    w_gate, w_up, w_down = expert_gate[0], expert_up[0], expert_down[0]
    width = w_gate.shape[1]
    chan = conv_out.shape[1]
    channels = chan * tp_count
    at = jnp.stack([lax.axis_index("tp"), lax.axis_index("sp")]).astype(jnp.int32)

    routes_t, weight_t = routes.T, route_weight.T
    sent = (experts, capacity, share)
    got_rows = sp_exchange(dispatch(at, routes_t, weight_t, expert_input, *sent, False))
    send_cots = dispatch(at, routes_t, weight_t, cotangent, *sent, True)
    got_cots = sp_exchange(send_cots)

    (picks,) = call(picks_body, at, (routes,), [((experts, tok_rows, capacity), bf16)])
    (own_stat,) = call(stats_body, at, (conv_out,), [((2, tok_rows), f32)])
    stats = [own_stat] + [tp_swap(own_stat, d) for d in (1, 2, 3)]
    value_scale, gate_scale = call(
        gates_body, at, (conv_value, conv_gate), [((tok_rows, chan), f32)] * 2
    )
    (mean_rstd,) = call(
        functools.partial(moments_body, chan=chan), at, stats, [((tok_rows, 2), f32)]
    )
    row_mean, row_rstd = mean_rstd[:, 0:1], mean_rstd[:, 1:2]
    norm_args = (conv_out, mean_rstd, norm_gain[None, :], norm_bias[None, :])

    half = experts // 2
    row_groups, cot_groups, pre, acts = [], [], [], []
    for g in range(2):
        row_groups.append(tp_pieces(jnp.stack(got_rows[g * half : (g + 1) * half])))
    for g in range(2):
        pre.append(pre_acts(at, row_groups[g], w_gate, w_up))
    for g in range(2):
        cot_groups.append(tp_pieces(jnp.stack(got_cots[g * half : (g + 1) * half])))
    for g in range(2):
        acts.append(hidden_grads(at, cot_groups[g], w_down, *pre[g]))
    hiddens, gate_pres, up_pres = ([a[i] for a in acts] for i in range(3))

    chunks = 2 if eighth % 256 == 0 else 1
    parts = [chunk_parts(share, eighth, c, chunks) for c in range(chunks)]
    cols = share // chunks
    resid_pieces, arrived = [], []
    sums = [[None, None] for _ in range(chunks)]
    for g in range(2):
        slots = slot_grads(at, gate_pres[g], up_pres[g], w_gate, w_up, parts)
        for c in range(chunks):
            own, near, far = slots[3 * c : 3 * c + 3]
            near = tp_swap(near, 1)
            far = (far.astype(f32) + near[:half].astype(f32)).astype(bf16)
            sums[c][g] = (own, near, tp_swap(far, 2))
    backs = []
    add = functools.partial(add_body, groups=2)
    for c in range(chunks):
        args = (*sums[c][0], *sums[c][1])
        totals = call(add, at, args, [((capacity, cols), bf16)] * experts)
        backs.append(sp_exchange(totals))
    wide = []
    for sides in (gate_pres, up_pres):
        wide += call(
            functools.partial(wide_body, groups=2),
            at,
            (*row_groups[0], *row_groups[1], *sides),
            [((model_width, width), f32)],
        )
    gate_grad, up_grad = wide
    (down_grad,) = call(
        functools.partial(down_body, groups=2),
        at,
        (*cot_groups[0], *cot_groups[1], *hiddens),
        [((width, model_width), f32)],
        keep=False,
    )
    for c in range(chunks):
        own = combine(at, picks, cotangent, backs[c], parts[c], share)
        resid_pieces.append(tp_pieces(own))
        (projected,) = call(
            owg_body,
            at,
            (*resid_pieces[c], *norm_args),
            [((sp_count, chan, eighth // chunks), bf16)],
        )
        arrived.append(sp_all(projected))
    resid_grad, norm_grad, own_sums = call(
        functools.partial(mix_body, parts=parts),
        at,
        (*[p for pieces in resid_pieces for p in pieces], out_weight, *norm_args),
        [((tok_rows, model_width), bf16), ((tok_rows, chan), f32), ((2, tok_rows), f32)],
    )
    others = [tp_swap(own_sums, d) for d in (1, 2, 3)]
    out_weight_grad = jnp.concatenate([jnp.sum(a.astype(f32), axis=0) for a in arrived], axis=1)

    taps_count = conv_taps.shape[0]
    all_sums = own_sums + others[0] + others[1] + others[2]
    normed = (conv_out.astype(f32) - row_mean) * row_rstd
    conv_grad = row_rstd * (
        norm_grad
        - (all_sums[0] / channels)[:, None]
        - normed * (all_sums[1] / channels)[:, None]
    )
    next_rows = passed_along(conv_grad[: taps_count - 1], "sp", -1)
    extended = jnp.concatenate([conv_grad, next_rows], axis=0)
    glu_grad = jnp.zeros_like(conv_grad)
    for lag_index in range(taps_count):
        begin = taps_count - 1 - lag_index
        glu_grad = glu_grad + conv_taps[lag_index][None, :] * extended[begin : begin + tok_rows]
    value_grad = (glu_grad * value_scale).astype(bf16)
    gate_in_grad = (glu_grad * gate_scale).astype(bf16)
    return (
        gate_grad[None],
        up_grad[None],
        down_grad[None],
        resid_grad,
        out_weight_grad,
        value_grad,
        gate_in_grad,
    )


def solution(mesh):
    return jax.shard_map(
        on_device,
        mesh=mesh,
        in_specs=(
            P("sp", None),
            P("sp", None),
            P("sp", None),
            P("sp", None),
            P("sp", None, "tp"),
            P("sp", None, "tp"),
            P("sp", "tp", None),
            P("sp", "tp"),
            P("sp", "tp"),
            P("sp", "tp"),
            P(None, "tp"),
            P("tp"),
            P("tp"),
            P("tp", None),
        ),
        out_specs=(
            P("sp", None, "tp"),
            P("sp", None, "tp"),
            P("sp", "tp", None),
            P("sp", None),
            P("tp", "sp"),
            P("sp", "tp"),
            P("sp", "tp"),
        ),
        check_vma=False,
    )
```

```python
import functools
import math

import jax
import jax.numpy as jnp
from jax import lax
from jax.experimental import pallas as pl
from jax.experimental.pallas import tpu as pltpu
from jax.sharding import PartitionSpec as P


norm_eps = 1e-06
f32 = jnp.float32
bf16 = jnp.bfloat16


def mm(a, b, ca, cb):
    return lax.dot_general(a, b, (((ca,), (cb,)), ((), ())), preferred_element_type=f32)


def exact_mm(a, b, ca, cb):
    return lax.dot_general(
        a, b, (((ca,), (cb,)), ((), ())), preferred_element_type=f32, precision=lax.Precision.HIGHEST
    )


def params(blocks, copies):
    if copies == 0:
        return pltpu.CompilerParams(vmem_limit_bytes=56 * 1024 * 1024)
    need = sum(math.prod(shape) * jnp.dtype(kind).itemsize for shape, kind in blocks)
    return pltpu.CompilerParams(vmem_limit_bytes=copies * need + 8 * 1024 * 1024)


def tp_swap(value, dist):
    count = lax.axis_size("tp")
    return lax.ppermute(value, "tp", [(i, i ^ dist) for i in range(count)])


def tp_pieces(own):
    far = tp_swap(own, 2)
    return (own, tp_swap(own, 1), far, tp_swap(far, 1))


def passed_along(value, axis, steps):
    count = lax.axis_size(axis)
    leading, last = (max(0, -steps), min(count, count - steps))
    return lax.ppermute(value, axis, [(source, source + steps) for source in range(leading, last)])


def dispatch_body(at_ref, routes_ref, weight_ref, source_ref, *outs, cots):
    experts, capacity = len(outs), outs[0].shape[0]
    top, tokens = routes_ref.shape
    expert_id = lax.broadcasted_iota(jnp.int32, (experts, tokens), 0)
    named = jnp.zeros((experts, tokens), f32)
    weights = jnp.zeros((experts, tokens), f32)
    for k in range(top):
        hit = (routes_ref[k : k + 1, :] ^ at_ref[1]) == expert_id
        named = jnp.where(hit, 1.0, named)
        weights = jnp.where(hit, weight_ref[k : k + 1, :], weights)
    before = lax.broadcasted_iota(jnp.int32, (tokens, tokens), 0) < lax.broadcasted_iota(
        jnp.int32, (tokens, tokens), 1
    )
    rank = mm(named.astype(bf16), jnp.where(before, 1.0, 0.0).astype(bf16), 1, 0)
    key = jnp.where(named > 0.5, rank, -1.0).astype(jnp.int32)
    slot = lax.broadcasted_iota(jnp.int32, (capacity, tokens), 0)
    for e in range(experts):
        pick = slot == key[e : e + 1, :]
        rows = mm(jnp.where(pick, 1.0, 0.0).astype(bf16), source_ref[...], 1, 0)
        if cots:
            rows = rows * jnp.sum(jnp.where(pick, weights[e : e + 1, :], 0.0), axis=1, keepdims=True)
        outs[e][...] = rows.astype(bf16)


def whole_spec(shape):
    return pl.BlockSpec(shape, lambda i, at: (0,) * len(shape))


def quarter_spec(tokens, share):
    return pl.BlockSpec((tokens, share), lambda i, at: (0, at[0]))


def call(body, at, args, outs, in_specs=None, out_specs=None, steps=1, keep=True):
    in_specs = in_specs or [whole_spec(a.shape) for a in args]
    out_specs = out_specs or [whole_spec(s) for s, _ in outs]
    blocks = [(spec.block_shape, a.dtype) for spec, a in zip(in_specs, args)]
    blocks += [(spec.block_shape, kind) for spec, (_, kind) in zip(out_specs, outs)]
    return pl.pallas_call(
        body,
        grid_spec=pltpu.PrefetchScalarGridSpec(
            num_scalar_prefetch=1, grid=(steps,), in_specs=in_specs, out_specs=out_specs
        ),
        out_shape=[jax.ShapeDtypeStruct(s, d) for s, d in outs],
        compiler_params=params(blocks, keep * min(steps, 2)),
    )(at, *args)


def dispatch(at, routes_t, weight_t, source, experts, capacity, share, cots):
    outs = [((capacity, share), bf16)] * experts
    return call(
        functools.partial(dispatch_body, cots=cots),
        at,
        (routes_t, weight_t, source),
        outs,
        [whole_spec(routes_t.shape), whole_spec(weight_t.shape), quarter_spec(source.shape[0], share)],
        keep=cots,
    )


def sp_swap(value, dist):
    count = lax.axis_size("sp")
    return lax.ppermute(value, "sp", [(i, i ^ dist) for i in range(count)])


def sp_exchange(blocks):
    got = list(blocks)
    for k in range(1, len(blocks)):
        got[k] = sp_swap(blocks[k], k)
    return got


def sp_all(value):
    return lax.all_to_all(value, "sp", split_axis=0, concat_axis=0, tiled=True)


def join(blocks):
    return jnp.concatenate(blocks, axis=0)


def rows_of(ref):
    return join([ref[i] for i in range(ref.shape[0])])


def store_blocks(ref, value, first=0, count=None):
    capacity = ref.shape[1]
    for i in range(ref.shape[0] if count is None else count):
        ref[first + i] = value[i * capacity : (i + 1) * capacity]


def pre_body(at_ref, p0, p1, p2, p3, wg_ref, wu_ref, gate_ref, up_ref):
    share = p0.shape[2]
    gate, up = 0.0, 0.0
    for j, piece in enumerate((p0, p1, p2, p3)):
        at = pl.ds(pl.multiple_of((at_ref[0] ^ j) * share, share), share)
        rows = rows_of(piece)
        gate = gate + mm(rows, wg_ref[at, :], 1, 0)
        up = up + mm(rows, wu_ref[at, :], 1, 0)
    store_blocks(gate_ref, gate)
    store_blocks(up_ref, up)


def blocked(shape):
    return pl.BlockSpec((2, *shape[1:]), lambda i, at: (i, 0, 0))


def pre_acts(at, pieces, w_gate, w_up):
    count, capacity, _ = pieces[0].shape
    mid = (count, capacity, w_gate.shape[1])
    return call(
        pre_body,
        at,
        (*pieces, w_gate, w_up),
        [(mid, f32)] * 2,
        [blocked(pieces[0].shape)] * 4 + [whole_spec(w_gate.shape)] * 2,
        [blocked(mid)] * 2,
        count // 2,
    )


def hidden_body(at_ref, p0, p1, p2, p3, wd_ref, gate_ref, up_ref, hid_ref, gp_ref, up_out_ref):
    share = p0.shape[2]
    grad = 0.0
    for j, piece in enumerate((p0, p1, p2, p3)):
        at = pl.ds(pl.multiple_of((at_ref[0] ^ j) * share, share), share)
        grad = grad + mm(rows_of(piece), wd_ref[:, at], 1, 1)
    gate = rows_of(gate_ref)
    up = rows_of(up_ref)
    sig = jax.nn.sigmoid(gate)
    act = gate * sig
    store_blocks(hid_ref, (act * up).astype(bf16))
    store_blocks(gp_ref, (grad * up * sig * (1.0 + gate * (1.0 - sig))).astype(bf16))
    store_blocks(up_out_ref, (grad * act).astype(bf16))


def hidden_grads(at, pieces, w_down, gate, up):
    count, capacity, _ = pieces[0].shape
    mid = (count, capacity, w_down.shape[0])
    return call(
        hidden_body,
        at,
        (*pieces, w_down, gate, up),
        [(mid, bf16)] * 3,
        [blocked(pieces[0].shape)] * 4 + [whole_spec(w_down.shape)] + [blocked(mid)] * 2,
        [blocked(mid)] * 3,
        count // 2,
    )


def chunk_parts(share, eighth, chunk, chunks):
    sub = eighth // chunks
    return [(b * eighth + chunk * sub, sub) for b in range(share // eighth)]


def slot_body(at_ref, gp_ref, up_ref, wg_ref, wu_ref, *outs, parts):
    share = wg_ref.shape[0] // 4
    count = gp_ref.shape[0]
    gp = rows_of(gp_ref)
    up = rows_of(up_ref)
    for c, spans in enumerate(parts):
        own_ref, near_ref, far_ref = outs[3 * c : 3 * c + 3]
        for j, out, first in ((3, near_ref, 0), (2, far_ref, 0), (1, near_ref, count), (0, own_ref, 0)):
            base = (at_ref[0] ^ j) * share
            rows = [pl.ds(pl.multiple_of(base + lo, size), size) for lo, size in spans]
            part = mm(gp, join([wg_ref[r, :] for r in rows]), 1, 1)
            part = part + mm(up, join([wu_ref[r, :] for r in rows]), 1, 1)
            store_blocks(out, part.astype(bf16), first, count)


def slot_grads(at, gate_pre, up_pre, w_gate, w_up, parts):
    count, capacity, _ = gate_pre.shape
    cols = sum(size for _, size in parts[0])
    one, two = (count, capacity, cols), (2 * count, capacity, cols)
    return call(
        functools.partial(slot_body, parts=parts),
        at,
        (gate_pre, up_pre, w_gate, w_up),
        [(one, bf16), (two, bf16), (one, bf16)] * len(parts),
    )


def add_body(at_ref, *refs, groups):
    ins, outs = refs[: 3 * groups], refs[3 * groups :]
    for g in range(groups):
        own, near, far = ins[3 * g : 3 * g + 3]
        count = own.shape[0]
        for i in range(count):
            total = own[i].astype(f32) + near[count + i].astype(f32) + far[i].astype(f32)
            outs[g * count + i][...] = total.astype(bf16)


def wide_body(at_ref, *refs, groups):
    pieces, refs = refs[: 4 * groups], refs[4 * groups :]
    gps, ups = refs[:groups], refs[groups : 2 * groups]
    gg_ref, ug_ref = refs[2 * groups :]
    share = pieces[0].shape[2]
    gp = join([rows_of(ref) for ref in gps])
    up = join([rows_of(ref) for ref in ups])
    for j in range(4):
        at = pl.ds(pl.multiple_of((at_ref[0] ^ j) * share, share), share)
        rows = join([rows_of(pieces[4 * g + j]) for g in range(groups)])
        gg_ref[at, :] = mm(rows, gp, 0, 0)
        ug_ref[at, :] = mm(rows, up, 0, 0)


def down_body(at_ref, *refs, groups):
    pieces, hids, dg_ref = refs[: 4 * groups], refs[4 * groups : 5 * groups], refs[5 * groups]
    share = pieces[0].shape[2]
    hid = join([rows_of(ref) for ref in hids])
    for j in range(4):
        at = pl.ds(pl.multiple_of((at_ref[0] ^ j) * share, share), share)
        rows = join([rows_of(pieces[4 * g + j]) for g in range(groups)])
        dg_ref[:, at] = mm(hid, rows, 0, 0)


def picks_body(at_ref, routes_ref, out_ref):
    experts, tokens, capacity = out_ref.shape
    top = routes_ref.shape[1]
    expert_id = lax.broadcasted_iota(jnp.int32, (tokens, experts), 1)
    named = jnp.zeros((tokens, experts), f32)
    for k in range(top):
        named = jnp.where((routes_ref[:, k : k + 1] ^ at_ref[1]) == expert_id, 1.0, named)
    before = lax.broadcasted_iota(jnp.int32, (tokens, tokens), 1) < lax.broadcasted_iota(
        jnp.int32, (tokens, tokens), 0
    )
    rank = mm(jnp.where(before, 1.0, 0.0).astype(bf16), named.astype(bf16), 1, 0)
    key = jnp.where(named > 0.5, rank, -1.0).astype(jnp.int32)
    slot = lax.broadcasted_iota(jnp.int32, (tokens, capacity), 1)
    for e in range(experts):
        out_ref[e] = jnp.where(slot == key[:, e : e + 1], 1.0, 0.0).astype(bf16)


def combine_body(at_ref, picks_ref, cot_ref, *refs, parts):
    backs, out_ref = refs[:-1], refs[-1]
    total = 0.0
    for e in range(picks_ref.shape[0]):
        total = total + mm(picks_ref[e], backs[e][...], 1, 0)
    cot = jnp.concatenate([cot_ref[:, lo : lo + size] for lo, size in parts], axis=1)
    out_ref[...] = (cot.astype(f32) + total).astype(bf16)


def combine(at, picks, cotangent, back, parts, share):
    tokens = cotangent.shape[0]
    (out,) = call(
        functools.partial(combine_body, parts=parts),
        at,
        (picks, cotangent, *back),
        [((tokens, back[0].shape[-1]), bf16)],
        [whole_spec(picks.shape), quarter_spec(tokens, share)] + [whole_spec(b.shape) for b in back],
    )
    return out


def stats_body(at_ref, conv_ref, out_ref):
    vals = conv_ref[...].astype(f32)
    mean = jnp.mean(vals, axis=1, keepdims=True)
    ones = jnp.ones((2, vals.shape[1]), f32)
    means = exact_mm(ones, vals, 1, 1) * (1.0 / vals.shape[1])
    squares = exact_mm(ones, (vals - mean) ** 2, 1, 1)
    row = lax.broadcasted_iota(jnp.int32, means.shape, 0)
    out_ref[...] = jnp.where(row == 0, means, squares)


def moments_body(at_ref, *refs, chan):
    stats, out_ref = [ref[...] for ref in refs[:-1]], refs[-1]
    count = len(stats)
    mean = sum(s[0:1] for s in stats) / count
    m2 = sum(s[1:2] + chan * (s[0:1] - mean) ** 2 for s in stats)
    rstd = lax.rsqrt(m2 / (count * chan) + norm_eps)
    row = lax.broadcasted_iota(jnp.int32, (2, mean.shape[1]), 0)
    both = jnp.where(row == 0, mean, rstd)
    out_ref[...] = exact_mm(both, jnp.eye(2, dtype=f32), 0, 0)


def norm_parts(conv_ref, mean_ref, gain_ref, bias_ref):
    normed = (conv_ref[...].astype(f32) - mean_ref[:, 0:1]) * mean_ref[:, 1:2]
    pre = normed * gain_ref[...] + bias_ref[...]
    sig = jax.nn.sigmoid(pre)
    return normed, pre, sig


def mix_body(at_ref, *refs, parts):
    pieces, refs = refs[: 4 * len(parts)], refs[4 * len(parts) :]
    w_ref, conv_ref, mean_ref, gain_ref, bias_ref, resid_ref, ng_ref, sums_ref = refs
    share = resid_ref.shape[1] // 4
    for c, spans in enumerate(parts):
        for j in range(4):
            base = (at_ref[0] ^ j) * share
            rows = pieces[4 * c + j]
            if len(parts) == 1:
                resid_ref[:, pl.ds(pl.multiple_of(base, share), share)] = rows[...]
                continue
            for b, (lo, size) in enumerate(spans):
                at = pl.ds(pl.multiple_of(base + lo, size), size)
                resid_ref[:, at] = rows[:, b * size : (b + 1) * size]
    mix = mm(resid_ref[...], w_ref[...], 1, 1)
    normed, pre, sig = norm_parts(conv_ref, mean_ref, gain_ref, bias_ref)
    grad = mix * sig * (1.0 + pre * (1.0 - sig)) * gain_ref[...]
    ng_ref[...] = grad
    ones = jnp.ones((2, grad.shape[1]), f32)
    total = exact_mm(ones, grad, 1, 1)
    dot = exact_mm(ones, grad * normed, 1, 1)
    row = lax.broadcasted_iota(jnp.int32, total.shape, 0)
    sums_ref[...] = jnp.where(row == 0, total, dot)


def gates_body(at_ref, value_ref, gate_ref, a_ref, b_ref):
    sig = jax.nn.sigmoid(gate_ref[...].astype(f32))
    a_ref[...] = sig
    b_ref[...] = value_ref[...].astype(f32) * sig * (1.0 - sig)


def owg_body(at_ref, p0, p1, p2, p3, conv_ref, mean_ref, gain_ref, bias_ref, out_ref):
    blocks, _, cols = out_ref.shape
    per = blocks // 4
    _, pre, sig = norm_parts(conv_ref, mean_ref, gain_ref, bias_ref)
    act = (pre * sig).astype(bf16)
    for j, piece in enumerate((p0, p1, p2, p3)):
        part = mm(act, piece[...], 0, 0).astype(bf16)
        for b in range(per):
            out_ref[(at_ref[0] ^ j) * per + b] = part[:, b * cols : (b + 1) * cols]


def on_device(
    expert_input,
    cotangent,
    routes,
    route_weight,
    expert_gate,
    expert_up,
    expert_down,
    conv_out,
    conv_value,
    conv_gate,
    conv_taps,
    norm_gain,
    norm_bias,
    out_weight,
):
    sp_count = lax.axis_size("sp")
    tp_count = lax.axis_size("tp")
    assert tp_count == 4 and expert_gate.shape[0] == 1
    tok_rows, model_width = expert_input.shape
    share = model_width // tp_count
    eighth = model_width // sp_count
    top_count = routes.shape[1]
    experts = sp_count
    capacity = 3 * top_count * tok_rows // (2 * experts)
    w_gate, w_up, w_down = expert_gate[0], expert_up[0], expert_down[0]
    width = w_gate.shape[1]
    chan = conv_out.shape[1]
    channels = chan * tp_count
    at = jnp.stack([lax.axis_index("tp"), lax.axis_index("sp")]).astype(jnp.int32)

    routes_t, weight_t = routes.T, route_weight.T
    sent = (experts, capacity, share)
    got_rows = sp_exchange(dispatch(at, routes_t, weight_t, expert_input, *sent, False))
    send_cots = dispatch(at, routes_t, weight_t, cotangent, *sent, True)
    got_cots = sp_exchange(send_cots)

    (picks,) = call(picks_body, at, (routes,), [((experts, tok_rows, capacity), bf16)])
    (own_stat,) = call(stats_body, at, (conv_out,), [((2, tok_rows), f32)])
    stats = [own_stat] + [tp_swap(own_stat, d) for d in (1, 2, 3)]
    value_scale, gate_scale = call(
        gates_body, at, (conv_value, conv_gate), [((tok_rows, chan), f32)] * 2
    )
    (mean_rstd,) = call(
        functools.partial(moments_body, chan=chan), at, stats, [((tok_rows, 2), f32)]
    )
    row_mean, row_rstd = mean_rstd[:, 0:1], mean_rstd[:, 1:2]
    norm_args = (conv_out, mean_rstd, norm_gain[None, :], norm_bias[None, :])

    half = experts // 2
    row_groups, cot_groups, pre, acts = [], [], [], []
    for g in range(2):
        row_groups.append(tp_pieces(jnp.stack(got_rows[g * half : (g + 1) * half])))
    for g in range(2):
        pre.append(pre_acts(at, row_groups[g], w_gate, w_up))
    for g in range(2):
        cot_groups.append(tp_pieces(jnp.stack(got_cots[g * half : (g + 1) * half])))
    for g in range(2):
        acts.append(hidden_grads(at, cot_groups[g], w_down, *pre[g]))
    hiddens, gate_pres, up_pres = ([a[i] for a in acts] for i in range(3))

    chunks = 2 if eighth % 256 == 0 else 1
    parts = [chunk_parts(share, eighth, c, chunks) for c in range(chunks)]
    cols = share // chunks
    resid_pieces, arrived = [], []
    sums = [[None, None] for _ in range(chunks)]
    for g in range(2):
        slots = slot_grads(at, gate_pres[g], up_pres[g], w_gate, w_up, parts)
        for c in range(chunks):
            own, near, far = slots[3 * c : 3 * c + 3]
            near = tp_swap(near, 1)
            far = (far.astype(f32) + near[:half].astype(f32)).astype(bf16)
            sums[c][g] = (own, near, tp_swap(far, 2))
    backs = []
    add = functools.partial(add_body, groups=2)
    for c in range(chunks):
        args = (*sums[c][0], *sums[c][1])
        totals = call(add, at, args, [((capacity, cols), bf16)] * experts)
        backs.append(sp_exchange(totals))
    gate_grad, up_grad = call(
        functools.partial(wide_body, groups=2),
        at,
        (*row_groups[0], *row_groups[1], *gate_pres, *up_pres),
        [((model_width, width), f32)] * 2,
        keep=False,
    )
    (down_grad,) = call(
        functools.partial(down_body, groups=2),
        at,
        (*cot_groups[0], *cot_groups[1], *hiddens),
        [((width, model_width), f32)],
    )
    for c in range(chunks):
        own = combine(at, picks, cotangent, backs[c], parts[c], share)
        resid_pieces.append(tp_pieces(own))
        (projected,) = call(
            owg_body,
            at,
            (*resid_pieces[c], *norm_args),
            [((sp_count, chan, eighth // chunks), bf16)],
        )
        arrived.append(sp_all(projected))
    resid_grad, norm_grad, own_sums = call(
        functools.partial(mix_body, parts=parts),
        at,
        (*[p for pieces in resid_pieces for p in pieces], out_weight, *norm_args),
        [((tok_rows, model_width), bf16), ((tok_rows, chan), f32), ((2, tok_rows), f32)],
    )
    others = [tp_swap(own_sums, d) for d in (1, 2, 3)]
    out_weight_grad = jnp.concatenate([jnp.sum(a.astype(f32), axis=0) for a in arrived], axis=1)

    taps_count = conv_taps.shape[0]
    all_sums = own_sums + others[0] + others[1] + others[2]
    normed = (conv_out.astype(f32) - row_mean) * row_rstd
    conv_grad = row_rstd * (
        norm_grad
        - (all_sums[0] / channels)[:, None]
        - normed * (all_sums[1] / channels)[:, None]
    )
    next_rows = passed_along(conv_grad[: taps_count - 1], "sp", -1)
    extended = jnp.concatenate([conv_grad, next_rows], axis=0)
    glu_grad = jnp.zeros_like(conv_grad)
    for lag_index in range(taps_count):
        begin = taps_count - 1 - lag_index
        glu_grad = glu_grad + conv_taps[lag_index][None, :] * extended[begin : begin + tok_rows]
    value_grad = (glu_grad * value_scale).astype(bf16)
    gate_in_grad = (glu_grad * gate_scale).astype(bf16)
    return (
        gate_grad[None],
        up_grad[None],
        down_grad[None],
        resid_grad,
        out_weight_grad,
        value_grad,
        gate_in_grad,
    )


def solution(mesh):
    return jax.shard_map(
        on_device,
        mesh=mesh,
        in_specs=(
            P("sp", None),
            P("sp", None),
            P("sp", None),
            P("sp", None),
            P("sp", None, "tp"),
            P("sp", None, "tp"),
            P("sp", "tp", None),
            P("sp", "tp"),
            P("sp", "tp"),
            P("sp", "tp"),
            P(None, "tp"),
            P("tp"),
            P("tp"),
            P("tp", None),
        ),
        out_specs=(
            P("sp", None, "tp"),
            P("sp", None, "tp"),
            P("sp", "tp", None),
            P("sp", None),
            P("tp", "sp"),
            P("sp", "tp"),
            P("sp", "tp"),
        ),
        check_vma=False,
    )
```
